32 devices in a mesh: gr: 2 (over y), fs: 4 (over z), tp: 4 (over x, core).
Axes of the slice: x: 2, y: 2, z: 4, core: 2. Of those that a mesh axis runs over, the one named last changes fastest.
Arguments:
- prompt: bfloat16 [4096, 2048], P(('gr', 'fs')), may hold values from -6 to 6
- norm_gain: float32 [2048], P(('gr', 'fs')), may hold values from 0.1 to 1.9
- gate_master: float32 [32, 2048, 1024], P(None, ('gr', 'fs'), 'tp'), may hold values from -6 to 6
- up_master: float32 [32, 2048, 1024], P(None, ('gr', 'fs'), 'tp'), may hold values from -6 to 6
- down_master: float32 [32, 2048, 1024], P(None, ('gr', 'fs'), 'tp'), may hold values from -6 to 6
- routes: int32 [4096, 2], P(('gr', 'fs')), may hold values from 0 to 31, as said below
- route_weights: float32 [4096, 2], P(('gr', 'fs')), may hold values from 0.1 to 0.9
Outputs:
- gate_ready: bfloat16 [32, 2048, 1024], P('fs', None, 'tp')
- up_ready: bfloat16 [32, 2048, 1024], P('fs', None, 'tp')
- down_ready: bfloat16 [32, 2048, 1024], P('fs', None, 'tp')
- blended: bfloat16 [4096, 2048], P(('gr', 'fs'), 'tp')
The draws below stay inside these ranges and needn't reach their ends.
Inputs may be any that keep to these rules, and one draw needn't show every extreme that they name: `routes`: each row names 2 different experts of one group: expert // 8 is the group. In every aligned block of 512 rows (the tokens of one index of gr and fs) half of the rows choose one group, and no expert is named more than 64 times; in every block some expert is named exactly 64 times.
All inputs are finite; a program needn't handle non-finite values.
Results may differ from the reference program's by a relative error of at most 0.015.
Values may be sent and summed in bfloat16 or wider, within the bound.
A program may use at most 128 MiB of HBM per device.

```python
import jax
import jax.numpy as jnp
from jax import lax

D = 2048
FF = 1024
N_GROUPS = 4
PER_GROUP = 8
TOP = 2
N_EXPERTS = 32
TOK_DEV = 512
CAP = 64
TOKENS = 4096
N_TP = 4


def draw_routes(key, part):
    blocks = TOKENS // TOK_DEV
    half_block = TOK_DEV // 2
    subkeys = jax.random.split(jax.random.fold_in(key, 7), 8)
    common = jax.random.randint(subkeys[0], (), 0, N_GROUPS)
    own_big = jax.random.randint(subkeys[1], (blocks,), 0, N_GROUPS)
    big_group = jnp.where(jnp.arange(blocks) < blocks // 2, common, own_big)
    cut_points = jnp.sort(jax.random.randint(subkeys[2], (blocks, N_GROUPS - 2), 0, half_block + 1), axis=1)
    edges = jnp.concatenate([jnp.zeros((blocks, 1), jnp.int32), cut_points.astype(jnp.int32), jnp.full((blocks, 1), half_block, jnp.int32)], axis=1)
    small_sizes = edges[:, 1:] - edges[:, :-1]
    groups = jnp.arange(N_GROUPS, dtype=jnp.int32)
    offset = (groups[None, :] - big_group[:, None] - 1) % N_GROUPS
    group_sizes = jnp.where(offset == N_GROUPS - 1, half_block, jnp.take_along_axis(small_sizes, jnp.minimum(offset, N_GROUPS - 2), axis=1))
    group_ends = jnp.cumsum(group_sizes, axis=1)
    starts = group_ends - group_sizes
    token_ranks = jnp.argsort(jax.random.randint(subkeys[3], (blocks, TOK_DEV), 0, 1 << 20) * TOK_DEV + jnp.arange(TOK_DEV, dtype=jnp.int32)[None, :], axis=1)
    group_of = jnp.sum((token_ranks[:, :, None] >= group_ends[:, None, :]).astype(jnp.int32), axis=2)
    inner_rank = token_ranks - jnp.take_along_axis(starts, group_of, axis=1)
    first_shift = jax.random.randint(subkeys[4], (blocks, N_GROUPS), 0, PER_GROUP)
    second_step = jax.random.randint(subkeys[5], (blocks, N_GROUPS), 1, PER_GROUP)
    local_order = jnp.argsort(jax.random.randint(subkeys[6], (blocks, N_GROUPS, PER_GROUP), 0, 1 << 20) * PER_GROUP + jnp.arange(PER_GROUP, dtype=jnp.int32), axis=2)
    first_local = (inner_rank + jnp.take_along_axis(first_shift, group_of, axis=1)) % PER_GROUP
    second_local = (first_local + jnp.take_along_axis(second_step, group_of, axis=1)) % PER_GROUP
    group_table = local_order[jnp.arange(blocks)[:, None], group_of]
    local_pair = jnp.take_along_axis(group_table, jnp.stack([first_local, second_local], axis=2), axis=2)
    experts = group_of[:, :, None] * PER_GROUP + local_pair
    return experts.reshape(TOKENS, TOP).astype(jnp.int32)


def steps_of(own_key, extent, shards, least, largest):
    def one(dim, shards_of):
        heights = jax.random.uniform(jax.random.fold_in(jax.random.fold_in(own_key, 6), dim), (shards_of,), jnp.float32, least / len(shards), largest / len(shards))
        return jnp.repeat(jnp.exp(heights), extent[dim] // shards_of).reshape((-1,) + (1,) * (len(extent) - dim - 1))

    loudness = one(*shards[0])
    for cut in shards[1:]:
        loudness = loudness * one(*cut)
    return loudness


def gaussian(key, dims, width, reach, cuts=(), held_as=jnp.bfloat16):
    entries = jax.random.normal(key, dims, jnp.float32) * width
    if len(cuts) > 0:
        entries = steps_of(key, dims, cuts, -0.22, 0.18) * entries
    return jnp.clip(entries, min=-reach, max=reach).astype(held_as)


def setup_inputs(seed: int = 0) -> dict:
    streams_of = jax.random.split(jax.random.key(seed), 8)
    return {
        "prompt": gaussian(streams_of[0], (TOKENS, D), 1.0, 6.0, ((0, 8),)),
        "norm_gain": jnp.clip(1.0 + 0.18 * jax.random.normal(streams_of[1], (D,), jnp.float32), 0.1, 1.9),
        "gate_master": gaussian(streams_of[2], (N_EXPERTS, D, FF), 1.0, 6.0, ((1, 8), (2, 4)), jnp.float32),
        "up_master": gaussian(streams_of[3], (N_EXPERTS, D, FF), 1.0, 6.0, ((1, 8), (2, 4)), jnp.float32),
        "down_master": gaussian(streams_of[4], (N_EXPERTS, D, FF), 1.0, 6.0, ((1, 8), (2, 4)), jnp.float32),
        "routes": draw_routes(jax.random.fold_in(streams_of[7], 71), 0),
        "route_weights": jnp.clip(0.1 + 0.79999997 * jax.random.uniform(streams_of[6], (TOKENS, TOP), jnp.float32) ** steps_of(streams_of[6], (TOKENS, TOP), ((0, 8),), -0.2, 0.2), 0.1, 0.9),
    }


EPS = 1e-06

def reference(prompt, norm_gain, gate_master, up_master, down_master, routes, route_weights):
    gate_new = (norm_gain[None, :, None] * gate_master).astype(jnp.bfloat16)
    up_new = (norm_gain[None, :, None] * up_master).astype(jnp.bfloat16)
    down_new = down_master.astype(jnp.bfloat16)
    prompt_wide = prompt.astype(jnp.float32)
    normed = (prompt_wide * lax.rsqrt(lax.optimization_barrier(jnp.mean(prompt_wide * prompt_wide, axis=-1, keepdims=True)) + EPS)).astype(jnp.bfloat16)
    route_list = routes.reshape(-1).astype(jnp.int32)
    route_hits = (route_list[:, None] == jnp.arange(N_EXPERTS, dtype=jnp.int32)[None, :]).astype(jnp.int32)
    slot_rank = lax.optimization_barrier(jnp.sum((jnp.cumsum(route_hits, axis=0).astype(jnp.int32) - 1) * route_hits, axis=1)).astype(jnp.int32)
    expert_room = TOKENS // TOK_DEV * CAP
    slot_index = (route_list * expert_room + slot_rank).astype(jnp.int32)
    token_of = (jnp.arange(route_list.shape[0], dtype=jnp.int32) // TOP).astype(jnp.int32)
    slot_owner = jnp.zeros((N_EXPERTS * expert_room,), jnp.int32).at[slot_index].set(token_of)

    def expert(operands):
        row_ids, gate_rows, up_rows, down_rows = operands
        picked = normed[row_ids]
        pre_gate = jnp.dot(picked, gate_rows, preferred_element_type=jnp.float32) * D ** (-0.5)
        pre_up = jnp.dot(picked, up_rows, preferred_element_type=jnp.float32) * D ** (-0.5)
        hidden = (jax.nn.silu(pre_gate) * pre_up).astype(jnp.bfloat16)
        hidden_blocks = hidden.astype(jnp.float32).reshape(row_ids.shape[0], N_TP, FF // N_TP)
        down_blocks = down_rows.astype(jnp.float32).reshape(D, N_TP, FF // N_TP)
        partial_value = (jnp.einsum('rnf,dnf->rnd', hidden_blocks, down_blocks) * FF ** (-0.5)).astype(jnp.bfloat16)
        return lax.optimization_barrier(jnp.sum(partial_value.astype(jnp.float32), axis=1)).astype(jnp.bfloat16)
    results = lax.map(expert, (slot_owner.reshape(N_EXPERTS, expert_room), gate_new, up_new, down_new))
    per_choice = results.reshape(N_EXPERTS * expert_room, D)[slot_index].reshape(TOKENS, TOP, D)
    blended = lax.optimization_barrier(jnp.sum(per_choice.astype(jnp.float32) * route_weights[:, :, None], axis=1))
    return (gate_new, up_new, down_new, blended.astype(jnp.bfloat16))
```

```python
import functools

import jax
import jax.numpy as jnp
from jax import lax
from jax.experimental import pallas as pl
from jax.experimental.pallas import tpu as pltpu
from jax.sharding import PartitionSpec as P

EPS = 1e-06
GROUP = 8
MESH = pl.DeviceIdType.MESH
STEPS = ((0, 0), (1, 0), (0, 1), (1, 1), (2, 0), (2, 1))
SLOTS = 4


def kernel(
    dims, gain, gm, um, dm, tok, wsend, g_out, u_out, d_out, ans,
    stage, wb, x, w, gb, ub, db, hid, yr, ys,
    st_sem, zs, zr, vs, vr, own_sem, tzs, tzr, wzs, wzr, txs, txr, tw_sem, ld_sem, dl_sem,
    ps, pr, rs, rr, rl_sem,
):
    gr, fs, tp, experts, rows, width, cap, depth, hidden_all = dims
    me_g, me_f, me_t = lax.axis_index("gr"), lax.axis_index("fs"), lax.axis_index("tp")
    local = experts // fs
    half = local // 2
    quarter = depth // tp
    total = fs * cap
    tile = min(256, cap)
    piece_rows = max(rows, 128)
    per_owner = quarter // piece_rows
    masters, outs = (gm, um, dm), (g_out, u_out, d_out)

    def fs_at(k):
        return lax.rem(me_f + k, fs)

    def fs_from(k):
        return lax.rem(me_f + fs - k, fs)

    def gr_at(j):
        return lax.rem(me_g + j, gr)

    def remote(src, dst, ssem, rsem, where):
        return pltpu.make_async_remote_copy(
            src_ref=src, dst_ref=dst, send_sem=ssem, recv_sem=rsem,
            device_id=where, device_id_type=MESH,
        )

    def region(s, g, f):
        m, h = STEPS[s]
        at = pl.multiple_of((g * fs + f) * rows, rows)
        return outs[m].at[pl.ds(h * half, half), pl.ds(at, rows), :]

    barrier = pltpu.get_barrier_semaphore()
    for k in range(1, fs):
        pl.semaphore_signal(barrier, inc=1, device_id={"fs": fs_at(k)}, device_id_type=MESH)
    for j in range(1, gr):
        pl.semaphore_signal(barrier, inc=1, device_id={"gr": gr_at(j)}, device_id_type=MESH)
    for j in range(1, tp):
        pl.semaphore_signal(
            barrier, inc=1, device_id={"tp": lax.rem(me_t + j, tp)}, device_id_type=MESH
        )
    pl.semaphore_wait(barrier, (fs - 1) + (gr - 1) + (tp - 1))

    def x_block(f, t):
        return x.at[
            pl.ds(pl.multiple_of(f * cap, cap), cap),
            pl.ds(pl.multiple_of(t * quarter, quarter), quarter),
        ]

    def w_block(f):
        return w.at[pl.ds(pl.multiple_of(f * cap, cap), cap), :]

    items = [(s, k) for s in range(len(STEPS)) for k in range(fs)]

    def load(i):
        s, k = items[i]
        m, h = STEPS[s]
        return pltpu.make_async_copy(
            masters[m].at[pl.ds(fs_at(k) * local + h * half, half)],
            stage.at[i % SLOTS], st_sem.at[i % SLOTS],
        )

    for i in range(SLOTS):
        load(i).start()

    sends = []
    early = []
    for k in range(1, fs):
        dst = fs_at(k)
        c = remote(tok.at[(dst * local) // GROUP], x_block(me_f, me_t), tzs.at[k], tzr.at[k], {"fs": dst})
        c.start()
        sends.append(c)
        c = remote(wsend.at[dst], w_block(me_f), wzs.at[k], wzr.at[k], {"fs": dst})
        c.start()
        sends.append(c)
    own_tok = pltpu.make_async_copy(
        tok.at[(me_f * local) // GROUP], x_block(me_f, me_t), tw_sem.at[0]
    )
    own_tok.start()
    own_w = pltpu.make_async_copy(wsend.at[me_f], w_block(me_f), tw_sem.at[1])
    own_w.start()

    own_copies = {}

    def send_gr(s, k, src):
        f = fs_from(k)
        for j in range(1, gr):
            c = remote(src, region(s, me_g, f), vs.at[s, k, j - 1], vr.at[s, k, j - 1], {"gr": gr_at(j)})
            c.start()
            sends.append(c)

    for i, (s, k) in enumerate(items):
        m, h = STEPS[s]
        load(i).wait()

        def cast(e, carry, s=s, k=k, m=m, i=i):
            value = stage[i % SLOTS, e]
            if m < 2:
                value = gain[...] * value
            wb[s, k, e] = value.astype(jnp.bfloat16)
            return carry

        lax.fori_loop(0, half, cast, 0)
        if i + SLOTS < len(items):
            load(i + SLOTS).start()
        if k == 0:
            c = pltpu.make_async_copy(wb.at[s, 0], region(s, me_g, me_f), own_sem.at[s])
            c.start()
            own_copies[s] = c
            if m < 2:
                send_gr(s, 0, wb.at[s, 0])
        else:
            c = remote(wb.at[s, k], region(s, me_g, me_f), zs.at[s, k], zr.at[s, k], {"fs": fs_at(k)})
            c.start()
            sends.append(c)

    own_tok.wait()
    own_w.wait()
    for k in range(fs):
        f = fs_from(k)
        if k > 0:
            remote(x_block(f, me_t), x_block(f, me_t), tzs.at[k], tzr.at[k], {"fs": f}).wait_recv()
            remote(w_block(f), w_block(f), wzs.at[k], wzr.at[k], {"fs": f}).wait_recv()
        for j in range(1, tp):
            c = remote(
                x_block(f, me_t), x_block(f, me_t), txs.at[k, j], txr.at[k, j],
                {"tp": lax.rem(me_t + j, tp)},
            )
            c.start()
            early.append(c)

    def forward(s, k):
        f = fs_from(k)
        remote(region(s, me_g, f), region(s, me_g, f), zs.at[s, k], zr.at[s, k], {"fs": f}).wait_recv()
        send_gr(s, k, region(s, me_g, f))

    def arrived_gr(s, k):
        f = fs_from(k)
        for j in range(1, gr):
            g = lax.rem(me_g + gr - j, gr)
            remote(
                region(s, g, f), region(s, g, f), vs.at[s, k, j - 1], vr.at[s, k, j - 1], {"gr": g}
            ).wait_recv()

    def loads(e, slot):
        return (
            pltpu.make_async_copy(g_out.at[e], gb.at[slot], ld_sem.at[0, slot]),
            pltpu.make_async_copy(u_out.at[e], ub.at[slot], ld_sem.at[1, slot]),
        )

    def experts_of(h):
        first = h * half
        for c in loads(first, 0):
            c.start()

        def one(n, carry):
            slot = lax.rem(n, 2)
            e = first + n

            @pl.when(n + 1 < half)
            def _():
                for c in loads(e + 1, 1 - slot):
                    c.start()

            for c in loads(e, slot):
                c.wait()

            def block(r, carry):
                at = pl.ds(pl.multiple_of(r * tile, tile), tile)
                xs = x[at, :]
                pre_gate = jnp.dot(xs, gb[slot], preferred_element_type=jnp.float32) * depth ** (-0.5)
                pre_up = jnp.dot(xs, ub[slot], preferred_element_type=jnp.float32) * depth ** (-0.5)
                ws = w[at, :]
                lane = lax.broadcasted_iota(jnp.int32, ws.shape, 1)
                weight = jnp.sum(jnp.where(lane == e, ws, 0.0), axis=1, keepdims=True)
                value = pre_gate / (1.0 + jnp.exp(-pre_gate)) * pre_up * weight
                hid[e, at, :] = value.astype(jnp.bfloat16)
                return carry

            lax.fori_loop(0, total // tile, block, 0)
            return carry

        lax.fori_loop(0, half, one, 0)

    chunks = []

    def chunk(index):
        ci = len(chunks)
        at = pl.multiple_of(index * piece_rows, piece_rows)
        owner = index // per_owner
        piece = lax.rem(index, per_owner)
        slot = ci % 2
        c = pltpu.make_async_copy(d_out.at[:, pl.ds(at, piece_rows), :], db.at[slot], dl_sem.at[slot])
        c.start()
        c.wait()

        def block(r, carry):
            here = pl.ds(pl.multiple_of(r * tile, tile), tile)
            acc = jnp.zeros((tile, piece_rows), jnp.float32)
            for e in range(local):
                acc += lax.dot_general(
                    hid[e, here, :], db[slot, e], (((1,), (1,)), ((), ())),
                    preferred_element_type=jnp.float32,
                )
            x[here, pl.ds(at, piece_rows)] = (acc * hidden_all ** (-0.5)).astype(jnp.bfloat16)
            return carry

        lax.fori_loop(0, total // tile, block, 0)
        turn = lax.rem(me_t + tp - owner, tp)
        slot_of = lax.rem(turn + tp - 1, tp)
        away = turn != 0
        chunks.append((at, owner, piece, slot_of, away))

        @pl.when(away)
        def _():
            partial_copy(ci).start()

    def partial_copy(ci):
        at, owner, piece, slot_of, away = chunks[ci]
        return remote(
            x.at[:, pl.ds(at, piece_rows)],
            yr.at[slot_of, :, pl.ds(pl.multiple_of(piece * piece_rows, piece_rows), piece_rows)],
            ps.at[ci], pr.at[slot_of, piece], {"tp": owner},
        )

    for s in (0, 1, 2):
        for k in range(1, fs):
            forward(s, k)
    send_gr(4, 0, wb.at[4, 0])
    for k in range(fs):
        f = fs_from(k)
        for j in range(1, tp):
            t = lax.rem(me_t + tp - j, tp)
            remote(x_block(f, t), x_block(f, t), txs.at[k, j], txr.at[k, j], {"tp": t}).wait_recv()
    for s in (0, 1):
        own_copies[s].wait()
        for k in range(fs):
            arrived_gr(s, k)
    experts_of(0)
    for k in range(1, fs):
        forward(3, k)
    send_gr(5, 0, wb.at[5, 0])
    for s in (2, 3):
        own_copies[s].wait()
        for k in range(fs):
            arrived_gr(s, k)
    experts_of(1)
    for c in early:
        c.wait_send()
    own_copies[4].wait()
    own_copies[5].wait()
    apart = rows == piece_rows
    if apart:
        chunk(me_g * fs + me_f)
    for k in range(1, fs):
        forward(4, k)
        forward(5, k)
        if apart:
            chunk(me_g * fs + fs_from(k))
    for k in range(fs):
        arrived_gr(4, k)
        arrived_gr(5, k)
        for j in range(1, gr):
            if apart:
                chunk(lax.rem(me_g + gr - j, gr) * fs + fs_from(k))
    if not apart:
        for index in range(depth // piece_rows):
            chunk(jnp.int32(index))

    for j in range(1, tp):
        for p in range(per_owner):
            ref = yr.at[j - 1, :, pl.ds(p * piece_rows, piece_rows)]
            remote(
                ref, ref, rl_sem.at[1], pr.at[j - 1, p], {"tp": lax.rem(me_t + j, tp)}
            ).wait_recv()
    for k in list(range(1, fs)) + [0]:
        f = fs_at(k)
        at = pl.ds(pl.multiple_of(f * cap, cap), cap)
        value = x[at, pl.ds(pl.multiple_of(me_t * quarter, quarter), quarter)].astype(jnp.float32)
        for j in range(tp - 1):
            value += yr[j, at, :].astype(jnp.float32)
        ys[at, :] = value.astype(jnp.bfloat16)
        if k > 0:
            c = remote(ys.at[at, :], ans.at[me_f], rs.at[k], rr.at[k], {"fs": f})
            c.start()
            sends.append(c)
        else:
            own_ans = pltpu.make_async_copy(ys.at[at, :], ans.at[me_f], rl_sem.at[0])
            own_ans.start()
    for k in range(1, fs):
        f = fs_from(k)
        remote(ans.at[f], ans.at[f], rs.at[k], rr.at[k], {"fs": f}).wait_recv()
    own_ans.wait()
    for c in sends:
        c.wait_send()
    for ci in range(len(chunks)):
        @pl.when(chunks[ci][4])
        def _(ci=ci):
            partial_copy(ci).wait_send()


def per_device(prompt, norm_gain, gate_master, up_master, down_master, routes, route_weights):
    gr, fs, tp = lax.axis_size("gr"), lax.axis_size("fs"), lax.axis_size("tp")
    experts, rows, width = gate_master.shape
    tokens, depth = prompt.shape
    local = experts // fs
    half = local // 2
    groups = experts // GROUP
    cap = tokens // 2
    quarter = depth // tp
    total = fs * cap
    piece_rows = max(rows, 128)
    per_owner = quarter // piece_rows
    bf16, f32 = jnp.bfloat16, jnp.float32

    wide = prompt.astype(f32)
    scale = lax.rsqrt(jnp.mean(wide * wide, axis=-1, keepdims=True) + EPS)
    mine = lax.dynamic_slice_in_dim(prompt, lax.axis_index("tp") * quarter, quarter, 1)
    normed = (mine.astype(f32) * scale).astype(bf16)
    group = routes[:, 0] // GROUP
    hits = group[:, None] == jnp.arange(groups, dtype=jnp.int32)[None, :]
    order = jnp.arange(tokens, dtype=jnp.int32)
    before = (order[None, :] < order[:, None]).astype(bf16)
    counts = jnp.dot(before, hits.astype(bf16), preferred_element_type=f32)
    rank = jnp.sum(jnp.where(hits, counts, 0.0), axis=1).astype(jnp.int32)
    slot = group * cap + rank
    place = jnp.arange(groups * cap, dtype=jnp.int32)[:, None] == slot[None, :]
    packed = jnp.dot(place.astype(bf16), normed, preferred_element_type=f32).astype(bf16)
    packed = packed.reshape(groups, cap, quarter)
    named = jnp.arange(experts, dtype=jnp.int32)
    weights = jnp.sum(
        jnp.where(routes[:, :, None] == named[None, None, :], route_weights[:, :, None], 0.0), axis=1
    )
    packed_w = jnp.dot(place.astype(f32), weights, precision=lax.Precision.HIGHEST)
    packed_w = packed_w.reshape(groups, cap, experts)
    sent_w = jnp.stack(
        [
            jnp.pad(
                packed_w[(d * local) // GROUP, :, d * local : (d + 1) * local],
                ((0, 0), (0, 128 - local)),
            )
            for d in range(fs)
        ]
    )
    dims = (gr, fs, tp, experts, rows, width, cap, depth, width * tp)
    any_spec = pl.BlockSpec(memory_space=pl.ANY)
    ready = jax.ShapeDtypeStruct((local, gr * fs * rows, width), bf16)
    steps = len(STEPS)
    dma = pltpu.SemaphoreType.DMA
    gate_ready, up_ready, down_ready, answers = pl.pallas_call(
        functools.partial(kernel, dims),
        name="reshard_experts",
        out_shape=(ready, ready, ready, jax.ShapeDtypeStruct((fs, cap, quarter), bf16)),
        in_specs=[pl.BlockSpec(memory_space=pltpu.VMEM)] + [any_spec] * 5,
        out_specs=(any_spec,) * 4,
        scratch_shapes=[
            pltpu.VMEM((SLOTS, half, rows, width), f32),
            pltpu.VMEM((steps, fs, half, rows, width), bf16),
            pltpu.VMEM((total, depth), bf16),
            pltpu.VMEM((total, 128), f32),
            pltpu.VMEM((2, depth, width), bf16),
            pltpu.VMEM((2, depth, width), bf16),
            pltpu.VMEM((2, local, piece_rows, width), bf16),
            pltpu.VMEM((local, total, width), bf16),
            pltpu.VMEM((tp - 1, total, quarter), bf16),
            pltpu.VMEM((total, quarter), bf16),
            dma((SLOTS,)),
            dma((steps, fs)), dma((steps, fs)),
            dma((steps, fs, gr - 1)), dma((steps, fs, gr - 1)),
            dma((steps,)),
            dma((fs,)), dma((fs,)), dma((fs,)), dma((fs,)),
            dma((fs, tp)), dma((fs, tp)),
            dma((2,)),
            dma((2, 2)), dma((2,)),
            dma((tp * per_owner,)), dma((tp - 1, per_owner)),
            dma((fs,)), dma((fs,)), dma((2,)),
        ],
        compiler_params=pltpu.CompilerParams(
            collective_id=0, has_side_effects=True, vmem_limit_bytes=66000000
        ),
    )(norm_gain[:, None], gate_master, up_master, down_master, packed, sent_w)
    answers = answers.reshape(groups, fs // groups, cap, quarter)
    answers = jnp.sum(answers.astype(f32), axis=1).astype(bf16).reshape(groups * cap, quarter)
    back = (slot[:, None] == jnp.arange(groups * cap, dtype=jnp.int32)[None, :]).astype(bf16)
    blended = jnp.dot(back, answers, preferred_element_type=f32)
    return (gate_ready, up_ready, down_ready, blended.astype(bf16))


def solution(mesh):
    both = ("gr", "fs")
    in_specs = (
        P(both, None),
        P(both),
        P(None, both, "tp"),
        P(None, both, "tp"),
        P(None, both, "tp"),
        P(both, None),
        P(both, None),
    )
    out_specs = (
        P("fs", None, "tp"),
        P("fs", None, "tp"),
        P("fs", None, "tp"),
        P(both, "tp"),
    )
    return jax.shard_map(
        per_device, mesh=mesh, in_specs=in_specs, out_specs=out_specs, check_vma=False
    )
```

```python
import functools

import jax
import jax.numpy as jnp
from jax import lax
from jax.experimental import pallas as pl
from jax.experimental.pallas import tpu as pltpu
from jax.sharding import PartitionSpec as P

EPS = 1e-06
GROUP = 8
MESH = pl.DeviceIdType.MESH
STEPS = ((0, 0), (1, 0), (0, 1), (1, 1), (2, 0), (2, 1))
SLOTS = 4


def kernel(
    dims, gain, gm, um, dm, tok, wsend, g_out, u_out, d_out, ans,
    stage, wb, x, w, gb, ub, db, hid, yr, ys,
    st_sem, zs, zr, vs, vr, own_sem, tzs, tzr, wzs, wzr, txs, txr, tw_sem, ld_sem, dl_sem,
    ps, pr, rs, rr, rl_sem,
):
    gr, fs, tp, experts, rows, width, cap, depth, hidden_all = dims
    me_g, me_f, me_t = lax.axis_index("gr"), lax.axis_index("fs"), lax.axis_index("tp")
    local = experts // fs
    half = local // 2
    quarter = depth // tp
    total = fs * cap
    tile = min(256, cap)
    piece_rows = max(rows, 128)
    per_owner = quarter // piece_rows
    masters, outs = (gm, um, dm), (g_out, u_out, d_out)

    def fs_at(k):
        return lax.rem(me_f + k, fs)

    def fs_from(k):
        return lax.rem(me_f + fs - k, fs)

    def gr_at(j):
        return lax.rem(me_g + j, gr)

    def remote(src, dst, ssem, rsem, where):
        return pltpu.make_async_remote_copy(
            src_ref=src, dst_ref=dst, send_sem=ssem, recv_sem=rsem,
            device_id=where, device_id_type=MESH,
        )

    def region(s, g, f):
        m, h = STEPS[s]
        at = pl.multiple_of((g * fs + f) * rows, rows)
        return outs[m].at[pl.ds(h * half, half), pl.ds(at, rows), :]

    barrier = pltpu.get_barrier_semaphore()
    for k in range(1, fs):
        pl.semaphore_signal(barrier, inc=1, device_id={"fs": fs_at(k)}, device_id_type=MESH)
    for j in range(1, gr):
        pl.semaphore_signal(barrier, inc=1, device_id={"gr": gr_at(j)}, device_id_type=MESH)
    for j in range(1, tp):
        pl.semaphore_signal(
            barrier, inc=1, device_id={"tp": lax.rem(me_t + j, tp)}, device_id_type=MESH
        )
    pl.semaphore_wait(barrier, (fs - 1) + (gr - 1) + (tp - 1))

    def x_block(f, t):
        return x.at[
            pl.ds(pl.multiple_of(f * cap, cap), cap),
            pl.ds(pl.multiple_of(t * quarter, quarter), quarter),
        ]

    def w_block(f):
        return w.at[:, pl.ds(pl.multiple_of(f * cap, cap), cap)]

    if fs == 4:
        odd, side = lax.rem(me_f, 2), lax.rem(me_t, 2)
        near, far = 1 + 2 * odd, 3 - 2 * odd
        sending = [
            jnp.where(side == 0, 2, near), jnp.where(side == 0, far, 2), jnp.where(side == 0, near, far)
        ]
        hearing = [2, 1, 3]
    else:
        sending = list(range(1, fs))
        hearing = sending
    items = [(s, k) for s in range(4) for k in [0] + sending]
    items += [(s, k) for k in [0] + sending for s in (4, 5)]

    def load(i):
        s, k = items[i]
        m, h = STEPS[s]
        return pltpu.make_async_copy(
            masters[m].at[pl.ds(fs_at(k) * local + h * half, half)],
            stage.at[i % SLOTS], st_sem.at[i % SLOTS],
        )

    for i in range(SLOTS):
        load(i).start()

    sends = []
    early = []
    for k in range(1, fs):
        dst = fs_at(k)
        c = remote(tok.at[(dst * local) // GROUP], x_block(me_f, me_t), tzs.at[k], tzr.at[k], {"fs": dst})
        c.start()
        sends.append(c)
        c = remote(wsend.at[dst], w_block(me_f), wzs.at[k], wzr.at[k], {"fs": dst})
        c.start()
        sends.append(c)
    own_tok = pltpu.make_async_copy(
        tok.at[(me_f * local) // GROUP], x_block(me_f, me_t), tw_sem.at[0]
    )
    own_tok.start()
    own_w = pltpu.make_async_copy(wsend.at[me_f], w_block(me_f), tw_sem.at[1])
    own_w.start()

    own_copies = {}

    def send_gr(s, k, src):
        f = fs_from(k)
        for j in range(1, gr):
            c = remote(src, region(s, me_g, f), vs.at[s, k, j - 1], vr.at[s, k, j - 1], {"gr": gr_at(j)})
            c.start()
            sends.append(c)

    for i, (s, k) in enumerate(items):
        m, h = STEPS[s]
        load(i).wait()

        def cast(e, carry, s=s, k=k, m=m, i=i):
            value = stage[i % SLOTS, e]
            if m < 2:
                value = gain[...] * value
            wb[s, k, e] = value.astype(jnp.bfloat16)
            return carry

        lax.fori_loop(0, half, cast, 0)
        if i + SLOTS < len(items):
            load(i + SLOTS).start()
        if isinstance(k, int) and k == 0:
            c = pltpu.make_async_copy(wb.at[s, 0], region(s, me_g, me_f), own_sem.at[s])
            c.start()
            own_copies[s] = c
            if m < 2:
                send_gr(s, 0, wb.at[s, 0])
        else:
            c = remote(wb.at[s, k], region(s, me_g, me_f), zs.at[s, k], zr.at[s, k], {"fs": fs_at(k)})
            c.start()
            sends.append(c)

    own_tok.wait()
    own_w.wait()
    for k in range(fs):
        f = fs_from(k)
        if k > 0:
            remote(x_block(f, me_t), x_block(f, me_t), tzs.at[k], tzr.at[k], {"fs": f}).wait_recv()
            remote(w_block(f), w_block(f), wzs.at[k], wzr.at[k], {"fs": f}).wait_recv()
        for j in range(1, tp):
            c = remote(
                x_block(f, me_t), x_block(f, me_t), txs.at[k, j], txr.at[k, j],
                {"tp": lax.rem(me_t + j, tp)},
            )
            c.start()
            early.append(c)

    def forward(s, k):
        f = fs_from(k)
        remote(region(s, me_g, f), region(s, me_g, f), zs.at[s, k], zr.at[s, k], {"fs": f}).wait_recv()
        send_gr(s, k, region(s, me_g, f))

    def arrived_gr(s, k):
        f = fs_from(k)
        for j in range(1, gr):
            g = lax.rem(me_g + gr - j, gr)
            remote(
                region(s, g, f), region(s, g, f), vs.at[s, k, j - 1], vr.at[s, k, j - 1], {"gr": g}
            ).wait_recv()

    def loads(e, slot):
        return (
            pltpu.make_async_copy(g_out.at[e], gb.at[slot], ld_sem.at[0, slot]),
            pltpu.make_async_copy(u_out.at[e], ub.at[slot], ld_sem.at[1, slot]),
        )

    def experts_of(h):
        first = h * half
        for c in loads(first, 0):
            c.start()

        def one(n, carry):
            slot = lax.rem(n, 2)
            e = first + n

            @pl.when(n + 1 < half)
            def _():
                for c in loads(e + 1, 1 - slot):
                    c.start()

            for c in loads(e, slot):
                c.wait()

            def block(r, carry):
                at = pl.ds(pl.multiple_of(r * tile, tile), tile)
                xs = x[at, :]
                pre_gate = jnp.dot(xs, gb[slot], preferred_element_type=jnp.float32) * depth ** (-0.5)
                pre_up = jnp.dot(xs, ub[slot], preferred_element_type=jnp.float32) * depth ** (-0.5)
                ws = jnp.transpose(w[:, at])
                lane = lax.broadcasted_iota(jnp.int32, ws.shape, 1)
                weight = jnp.sum(jnp.where(lane == e, ws, 0.0), axis=1, keepdims=True)
                value = pre_gate / (1.0 + jnp.exp(-pre_gate)) * pre_up * weight
                hid[e, at, :] = value.astype(jnp.bfloat16)
                return carry

            lax.fori_loop(0, total // tile, block, 0)
            return carry

        lax.fori_loop(0, half, one, 0)

    chunks = []

    def chunk(index):
        ci = len(chunks)
        at = pl.multiple_of(index * piece_rows, piece_rows)
        owner = index // per_owner
        piece = lax.rem(index, per_owner)
        slot = ci % 2
        c = pltpu.make_async_copy(d_out.at[:, pl.ds(at, piece_rows), :], db.at[slot], dl_sem.at[slot])
        c.start()
        c.wait()

        def block(r, carry):
            here = pl.ds(pl.multiple_of(r * tile, tile), tile)
            acc = jnp.zeros((tile, piece_rows), jnp.float32)
            for e in range(local):
                acc += lax.dot_general(
                    hid[e, here, :], db[slot, e], (((1,), (1,)), ((), ())),
                    preferred_element_type=jnp.float32,
                )
            x[here, pl.ds(at, piece_rows)] = (acc * hidden_all ** (-0.5)).astype(jnp.bfloat16)
            return carry

        lax.fori_loop(0, total // tile, block, 0)
        turn = lax.rem(me_t + tp - owner, tp)
        slot_of = lax.rem(turn + tp - 1, tp)
        away = turn != 0
        chunks.append((at, owner, piece, slot_of, away))

        @pl.when(away)
        def _():
            partial_copy(ci).start()

        if ci >= 2:
            finish(ci - 2)

    def answer_part(p):
        return pl.ds(pl.multiple_of(p * piece_rows, piece_rows), piece_rows)

    def answer_copy(k, p):
        f = fs_at(k)
        at = pl.ds(pl.multiple_of(f * cap, cap), cap)
        return remote(
            ys.at[at, answer_part(p)], ans.at[me_f, :, answer_part(p)],
            rs.at[k, p], rr.at[k, p], {"fs": f},
        )

    def own_answer(p):
        at = pl.ds(pl.multiple_of(me_f * cap, cap), cap)
        return pltpu.make_async_copy(
            ys.at[at, answer_part(p)], ans.at[me_f, :, answer_part(p)], rl_sem.at[p]
        )

    def finish(ci):
        here, owner, p, slot_of, away = chunks[ci]

        @pl.when(jnp.logical_not(away))
        def _():
            for j in range(1, tp):
                ref = yr.at[j - 1, :, answer_part(p)]
                remote(
                    ref, ref, ps.at[ci], pr.at[j - 1, p], {"tp": lax.rem(me_t + j, tp)}
                ).wait_recv()
            for k in list(range(1, fs)) + [0]:
                at = pl.ds(pl.multiple_of(fs_at(k) * cap, cap), cap)
                value = x[at, pl.ds(here, piece_rows)].astype(jnp.float32)
                for j in range(tp - 1):
                    value += yr[j, at, answer_part(p)].astype(jnp.float32)
                ys[at, answer_part(p)] = value.astype(jnp.bfloat16)
                if k > 0:
                    answer_copy(k, p).start()
                else:
                    own_answer(p).start()

    def partial_copy(ci):
        at, owner, piece, slot_of, away = chunks[ci]
        return remote(
            x.at[:, pl.ds(at, piece_rows)],
            yr.at[slot_of, :, pl.ds(pl.multiple_of(piece * piece_rows, piece_rows), piece_rows)],
            ps.at[ci], pr.at[slot_of, piece], {"tp": owner},
        )

    for s in (0, 1, 2):
        for k in hearing:
            forward(s, k)
    send_gr(4, 0, wb.at[4, 0])
    for k in range(fs):
        f = fs_from(k)
        for j in range(1, tp):
            t = lax.rem(me_t + tp - j, tp)
            remote(x_block(f, t), x_block(f, t), txs.at[k, j], txr.at[k, j], {"tp": t}).wait_recv()
    for s in (0, 1):
        own_copies[s].wait()
        for k in range(fs):
            arrived_gr(s, k)
    experts_of(0)
    for k in hearing:
        forward(3, k)
    send_gr(5, 0, wb.at[5, 0])
    for s in (2, 3):
        own_copies[s].wait()
        for k in range(fs):
            arrived_gr(s, k)
    experts_of(1)
    for c in early:
        c.wait_send()
    own_copies[4].wait()
    own_copies[5].wait()
    apart = rows == piece_rows

    def others(k):
        arrived_gr(4, k)
        arrived_gr(5, k)
        if apart:
            for j in range(1, gr):
                chunk(lax.rem(me_g + gr - j, gr) * fs + fs_from(k))

    if apart:
        chunk(me_g * fs + me_f)
    last = 0
    for k in hearing:
        forward(4, k)
        forward(5, k)
        if apart:
            chunk(me_g * fs + fs_from(k))
        others(last)
        last = k
    others(last)
    if not apart:
        for index in range(depth // piece_rows):
            chunk(jnp.int32(index))

    for ci in range(max(0, len(chunks) - 2), len(chunks)):
        finish(ci)
    for p in range(per_owner):
        for k in range(1, fs):
            answer_copy(k, p).wait_send()
            f = fs_from(k)
            ref = ans.at[f, :, pl.ds(p * piece_rows, piece_rows)]
            remote(ref, ref, rs.at[k, p], rr.at[k, p], {"fs": f}).wait_recv()
        own_answer(p).wait()
    for c in sends:
        c.wait_send()
    for ci in range(len(chunks)):
        @pl.when(chunks[ci][4])
        def _(ci=ci):
            partial_copy(ci).wait_send()


def per_device(prompt, norm_gain, gate_master, up_master, down_master, routes, route_weights):
    gr, fs, tp = lax.axis_size("gr"), lax.axis_size("fs"), lax.axis_size("tp")
    experts, rows, width = gate_master.shape
    tokens, depth = prompt.shape
    local = experts // fs
    half = local // 2
    groups = experts // GROUP
    cap = tokens // 2
    quarter = depth // tp
    total = fs * cap
    piece_rows = max(rows, 128)
    per_owner = quarter // piece_rows
    bf16, f32 = jnp.bfloat16, jnp.float32

    wide = prompt.astype(f32)
    scale = lax.rsqrt(jnp.mean(wide * wide, axis=-1, keepdims=True) + EPS)
    mine = lax.dynamic_slice_in_dim(prompt, lax.axis_index("tp") * quarter, quarter, 1)
    normed = (mine.astype(f32) * scale).astype(bf16)
    group = routes[:, 0] // GROUP
    hits = group[:, None] == jnp.arange(groups, dtype=jnp.int32)[None, :]
    order = jnp.arange(tokens, dtype=jnp.int32)
    before = (order[None, :] < order[:, None]).astype(bf16)
    counts = jnp.dot(before, hits.astype(bf16), preferred_element_type=f32)
    rank = jnp.sum(jnp.where(hits, counts, 0.0), axis=1).astype(jnp.int32)
    slot = group * cap + rank
    place = jnp.arange(groups * cap, dtype=jnp.int32)[:, None] == slot[None, :]
    packed = jnp.dot(place.astype(bf16), normed, preferred_element_type=f32).astype(bf16)
    packed = packed.reshape(groups, cap, quarter)
    named = jnp.arange(experts, dtype=jnp.int32)
    weights = jnp.sum(
        jnp.where(routes[:, :, None] == named[None, None, :], route_weights[:, :, None], 0.0), axis=1
    )
    packed_w = jnp.dot(place.astype(f32), weights, precision=lax.Precision.HIGHEST)
    packed_w = packed_w.reshape(groups, cap, experts)
    sent_w = jnp.stack(
        [
            jnp.pad(
                packed_w[(d * local) // GROUP, :, d * local : (d + 1) * local],
                ((0, 0), (0, max(8, local) - local)),
            ).T
            for d in range(fs)
        ]
    )
    dims = (gr, fs, tp, experts, rows, width, cap, depth, width * tp)
    any_spec = pl.BlockSpec(memory_space=pl.ANY)
    ready = jax.ShapeDtypeStruct((local, gr * fs * rows, width), bf16)
    steps = len(STEPS)
    dma = pltpu.SemaphoreType.DMA
    gate_ready, up_ready, down_ready, answers = pl.pallas_call(
        functools.partial(kernel, dims),
        name="reshard_experts",
        out_shape=(ready, ready, ready, jax.ShapeDtypeStruct((fs, cap, quarter), bf16)),
        in_specs=[pl.BlockSpec(memory_space=pltpu.VMEM)] + [any_spec] * 5,
        out_specs=(any_spec,) * 4,
        scratch_shapes=[
            pltpu.VMEM((SLOTS, half, rows, width), f32),
            pltpu.VMEM((steps, fs, half, rows, width), bf16),
            pltpu.VMEM((total, depth), bf16),
            pltpu.VMEM((max(8, local), total), f32),
            pltpu.VMEM((2, depth, width), bf16),
            pltpu.VMEM((2, depth, width), bf16),
            pltpu.VMEM((2, local, piece_rows, width), bf16),
            pltpu.VMEM((local, total, width), bf16),
            pltpu.VMEM((tp - 1, total, quarter), bf16),
            pltpu.VMEM((total, quarter), bf16),
            dma((SLOTS,)),
            dma((steps, fs)), dma((steps, fs)),
            dma((steps, fs, gr - 1)), dma((steps, fs, gr - 1)),
            dma((steps,)),
            dma((fs,)), dma((fs,)), dma((fs,)), dma((fs,)),
            dma((fs, tp)), dma((fs, tp)),
            dma((2,)),
            dma((2, 2)), dma((2,)),
            dma((tp * per_owner,)), dma((tp - 1, per_owner)),
            dma((fs, per_owner)), dma((fs, per_owner)), dma((per_owner,)),
        ],
        compiler_params=pltpu.CompilerParams(
            collective_id=0, has_side_effects=True, vmem_limit_bytes=66000000
        ),
    )(norm_gain[:, None], gate_master, up_master, down_master, packed, sent_w)
    answers = answers.reshape(groups, fs // groups, cap, quarter)
    answers = jnp.sum(answers.astype(f32), axis=1).astype(bf16).reshape(groups * cap, quarter)
    back = (slot[:, None] == jnp.arange(groups * cap, dtype=jnp.int32)[None, :]).astype(bf16)
    blended = jnp.dot(back, answers, preferred_element_type=f32)
    return (gate_ready, up_ready, down_ready, blended.astype(bf16))


def solution(mesh):
    both = ("gr", "fs")
    in_specs = (
        P(both, None),
        P(both),
        P(None, both, "tp"),
        P(None, both, "tp"),
        P(None, both, "tp"),
        P(both, None),
        P(both, None),
    )
    out_specs = (
        P("fs", None, "tp"),
        P("fs", None, "tp"),
        P("fs", None, "tp"),
        P(both, "tp"),
    )
    return jax.shard_map(
        per_device, mesh=mesh, in_specs=in_specs, out_specs=out_specs, check_vma=False
    )
```
